32 devices in a mesh: grp: 2 (over x), tp: 4 (over z), dp: 4 (over y, core).
Axes of the slice: x: 2, y: 2, z: 4, core: 2. Of those that a mesh axis runs over, the one named last changes fastest.
Arguments:
- stream: bfloat16 [32, 4096], P('grp', 'dp'), parts along dimension 0, may hold values from -11 to 11
- states: float32 [2, 32, 32, 64, 64], P(None, ('grp', 'dp'), 'tp'), parts along dimension 1, may hold values from -6 to 6
- norm_gain: bfloat16 [2, 4096], P(None, 'dp'), may hold values from 0.099609375 to 1.8984375
- recept_weight: bfloat16 [2, 4096, 2048], P(None, 'dp', 'tp'), may hold values from -0.09375 to 0.09375
- key_weight: bfloat16 [2, 4096, 2048], P(None, 'dp', 'tp'), may hold values from -0.09375 to 0.09375
- value_weight: bfloat16 [2, 4096, 2048], P(None, 'dp', 'tp'), may hold values from -0.09375 to 0.09375
- decay_weight: bfloat16 [2, 4096, 2048], P(None, 'dp', 'tp'), may hold values from -0.09375 to 0.09375
- rate_weight: bfloat16 [2, 4096, 2048], P(None, 'dp', 'tp'), may hold values from -0.09375 to 0.09375
- gate_weight: bfloat16 [2, 4096, 2048], P(None, 'dp', 'tp'), may hold values from -0.09375 to 0.09375
- out_weight: bfloat16 [2, 2048, 4096], P(None, 'tp', 'dp'), may hold values from -0.125 to 0.125
- decay_bias: float32 [2, 2048], P(None, 'tp'), may hold values from -2 to 2
- head_gain: bfloat16 [2, 2048], P(None, 'tp'), may hold values from 0.099609375 to 1.8984375
Outputs:
- new_stream: bfloat16 [32, 4096], P('grp', 'dp'), parts along dimension 0
- new_states: float32 [2, 32, 32, 64, 64], P(None, ('grp', 'dp'), 'tp'), parts along dimension 1
The draws below stay inside these ranges and needn't reach their ends.
There are 2 independent parts, one for each index of `grp`. The reference program is written for one: setup_inputs(seed, part) draws one part's arguments, and reference() takes and returns one part's arrays. A program takes and returns all parts, laid end to end along the dimension named above; an argument that names none is the same for every part. Nothing has to cross between parts.
All inputs are finite; a program needn't handle non-finite values.
Results may differ from the reference program's by a relative error of at most 0.0068.
Values may be sent and summed in bfloat16 or wider, within the bound.
A program may use at most 64 MiB of HBM per device.

```python
import jax
import jax.numpy as jnp
from jax import lax

D = 4096
INNER = 2048
HEAD = 64
HEADS = 32
SEQS = 16


def draw_stream(key, part):
    first, second = jax.random.split(jax.random.fold_in(key, 11), 2)
    columns = jnp.arange(D, dtype=jnp.float32) / D
    rough = jax.random.uniform(second, (D,), jnp.float32, 0.5, 1.5)
    scales = 0.6 * jnp.power(3.0, columns) * rough
    base = jnp.clip(jax.random.normal(first, (SEQS, D), jnp.float32), -4.0, 4.0)
    values = base * scales[None, :]
    return jnp.clip(values, -11.0, 11.0).astype(jnp.bfloat16)


def levels(stream_key, shape, cuts, smallest, high):
    def one(axis_at, blocks):
        draws = jax.random.uniform(jax.random.fold_in(jax.random.fold_in(stream_key, 6), axis_at), (blocks,), jnp.float32, smallest / len(cuts), high / len(cuts))
        return jnp.repeat(jnp.exp(draws), shape[axis_at] // blocks).reshape((-1,) + (1,) * (len(shape) - axis_at - 1))

    level = one(*cuts[0])
    for cut in cuts[1:]:
        level = level * one(*cut)
    return level


def gaussian(rng, dims, deviation, bound, cuts=(), held_as=jnp.bfloat16):
    values = deviation * jax.random.normal(rng, dims, jnp.float32)
    if cuts:
        values = values * levels(rng, dims, cuts, -0.22, 0.18)
    return jnp.clip(values, -bound, bound).astype(held_as)


def setup_inputs(seed: int = 0, part: int = 0) -> dict:
    key_of = jax.random.split(jax.random.key(seed), 13)
    own_keys = jax.random.split(jax.random.fold_in(key_of[12], part), 13)
    stream = draw_stream(jax.random.fold_in(jax.random.fold_in(key_of[12], part), 71), part)
    states = gaussian(own_keys[1], (2, SEQS, HEADS, HEAD, HEAD), 0.5, 6.0, ((1, 4), (2, 4)), jnp.float32)
    norm_gain = jnp.clip(1.0 + 0.18 * jax.random.normal(key_of[2], (2, D), jnp.float32), 0.099609375, 1.8984375).astype(jnp.bfloat16)
    recept_weight = gaussian(key_of[3], (2, D, INNER), D ** -0.5, 0.09375, ((1, 4), (2, 4)))
    key_weight = gaussian(key_of[4], (2, D, INNER), D ** -0.5, 0.09375, ((1, 4), (2, 4)))
    value_weight = gaussian(key_of[5], (2, D, INNER), D ** -0.5, 0.09375, ((1, 4), (2, 4)))
    decay_weight = gaussian(key_of[6], (2, D, INNER), D ** -0.5, 0.09375, ((1, 4), (2, 4)))
    rate_weight = gaussian(key_of[7], (2, D, INNER), D ** -0.5, 0.09375, ((1, 4), (2, 4)))
    gate_weight = gaussian(key_of[8], (2, D, INNER), D ** -0.5, 0.09375, ((1, 4), (2, 4)))
    out_weight = gaussian(key_of[9], (2, INNER, D), INNER ** -0.5, 0.125, ((1, 4), (2, 4)))
    decay_bias = jnp.clip(jax.random.uniform(key_of[10], (2, INNER), jnp.float32, -2.0, 2.0) * levels(key_of[10], (2, INNER), ((1, 4),), -0.4, 0.0), -2.0, 2.0)
    head_gain = jnp.clip(1.0 + 0.18 * jax.random.normal(key_of[11], (2, INNER), jnp.float32), 0.099609375, 1.8984375).astype(jnp.bfloat16)
    return {"stream": stream, "states": states, "norm_gain": norm_gain, "recept_weight": recept_weight, "key_weight": key_weight, "value_weight": value_weight, "decay_weight": decay_weight, "rate_weight": rate_weight, "gate_weight": gate_weight, "out_weight": out_weight, "decay_bias": decay_bias, "head_gain": head_gain}


def run_block(stream, state_blk, gain, weights, out_weight, bias, hgain):
    current = stream.astype(jnp.float32)
    inv_rms = lax.rsqrt(lax.optimization_barrier(jnp.mean(current * current, axis=1, keepdims=True)) + 1e-06)
    normed = (current * gain.astype(jnp.float32)).astype(jnp.bfloat16)
    seqs = stream.shape[0]
    projected = [(jnp.dot(normed, weight, preferred_element_type=jnp.float32) * inv_rms).reshape(seqs, -1, HEAD) for weight in weights]
    recept, key_vec, value_vec, decay_pre, rate_pre, gate_pre = projected
    unit_key = key_vec * lax.rsqrt(lax.optimization_barrier(jnp.sum(key_vec * key_vec, axis=2, keepdims=True)) + 1e-06)
    rate_vec = jax.nn.sigmoid(rate_pre)
    decay = jnp.exp(-0.606531 * jax.nn.sigmoid(bias.reshape(1, -1, HEAD) + decay_pre))
    removed = jnp.einsum('bhij,bhj->bhi', state_blk, unit_key, precision=lax.Precision.HIGHEST)
    new_state = state_blk * decay[:, :, None, :] - removed[..., None] * (unit_key * rate_vec)[:, :, None, :] + value_vec[..., None] * key_vec[:, :, None, :]
    read = jnp.einsum('bhij,bhj->bhi', new_state, recept, precision=lax.Precision.HIGHEST)
    center = read - lax.optimization_barrier(jnp.mean(read, axis=2, keepdims=True))
    normal_read = center * lax.rsqrt(lax.optimization_barrier(jnp.mean(center * center, axis=2, keepdims=True)) + 1e-05)
    gated = normal_read * hgain.astype(jnp.float32).reshape(1, -1, HEAD) * jax.nn.sigmoid(gate_pre)
    mixed = gated.reshape(seqs, -1).astype(jnp.bfloat16)
    branch = jnp.dot(mixed, out_weight, preferred_element_type=jnp.float32)
    return ((current + branch).astype(jnp.bfloat16), new_state)

def reference(stream, states, norm_gain, recept_weight, key_weight, value_weight, decay_weight, rate_weight, gate_weight, out_weight, decay_bias, head_gain):
    current = stream
    fresh_list = []
    for layer in range(2):
        weights = (recept_weight[layer], key_weight[layer], value_weight[layer], decay_weight[layer], rate_weight[layer], gate_weight[layer])
        current, fresh = run_block(current, states[layer], norm_gain[layer], weights, out_weight[layer], decay_bias[layer], head_gain[layer])
        fresh_list.append(fresh)
    return (current, jnp.stack(fresh_list))
```

```python
import functools

import jax
import jax.numpy as jnp
from jax import lax
from jax.experimental import pallas as pl
from jax.experimental.pallas import tpu as pltpu
from jax.sharding import PartitionSpec as P

F32 = jnp.float32
BF16 = jnp.bfloat16
MESH = pl.DeviceIdType.MESH
LANES = 128
ROLES = 6
KEY, RECEPT, DECAY, RATE, VALUE, GATE = range(ROLES)
PAIRS = ROLES // 2


def split2(x):
    high = x.astype(BF16).astype(F32)
    return jnp.concatenate([high, x - high], axis=0)


def kernel(
    n_dp, n_tp, width_all,
    stream, states, gain, rw, kw, vw, dw, tw, gw, ow, bias, hgain,
    out_stream, out_states,
    st_v, s_v, so_v, sb_v, gain_v, w_v, ow_v, bias_v, hgain_v, fin_v,
    proj_s, proj_r, sq_s, sq_r, mix_s, mix_r, br_s, br_r,
    small_sem, w_sem, ow_sem, s_sem, so_sem, fin_sem,
    pj_ss, pj_rs, sq_ss, sq_rs, mx_ss, mx_rs, br_ss, br_rs,
):
    dp = lax.axis_index("dp")
    tp = lax.axis_index("tp")
    seqs, cols = stream.shape
    layers, local, heads, head, _ = states.shape
    width = heads * head
    groups = width // LANES
    rows = groups * local

    small = [
        pltpu.make_async_copy(src, dst, small_sem.at[i])
        for i, (src, dst) in enumerate(
            [(stream, st_v), (gain, gain_v), (bias, bias_v), (hgain, hgain_v)]
        )
    ]
    weights = (kw, rw, dw, tw, vw, gw)
    w_copy = [
        [pltpu.make_async_copy(weights[r].at[l], w_v.at[l, r], w_sem.at[l, r]) for r in range(ROLES)]
        for l in range(layers)
    ]
    ow_copy = [pltpu.make_async_copy(ow.at[l], ow_v.at[l], ow_sem.at[l]) for l in range(layers)]
    s_copy = [pltpu.make_async_copy(states.at[l], s_v.at[l], s_sem.at[l]) for l in range(layers)]
    for copy in small:
        copy.start()
    for copy in w_copy[0]:
        copy.start()

    barrier = pltpu.get_barrier_semaphore()
    for k in range(1, n_dp):
        pl.semaphore_signal(barrier, inc=1, device_id={"dp": lax.rem(dp + k, n_dp)}, device_id_type=MESH)
    for k in range(1, n_tp):
        pl.semaphore_signal(barrier, inc=1, device_id={"tp": lax.rem(tp + k, n_tp)}, device_id_type=MESH)

    lane_r = lax.broadcasted_iota(jnp.int32, (LANES, LANES), 0)
    lane_c = lax.broadcasted_iota(jnp.int32, (LANES, LANES), 1)
    same_head = jnp.where((lane_r < head) == (lane_c < head), 1.0, 0.0).astype(BF16)

    def head_sum(x):
        both = jnp.dot(split2(x).astype(BF16), same_head, preferred_element_type=F32)
        return both[: x.shape[0]] + both[x.shape[0]:]

    first_head = lax.broadcasted_iota(jnp.int32, (2 * rows, LANES), 1) < head
    pair_row = lax.broadcasted_iota(jnp.int32, (2 * rows, LANES), 0)

    def fold(row):
        return jnp.concatenate(
            [jnp.broadcast_to(row[:, g * LANES:(g + 1) * LANES], (local, LANES)) for g in range(groups)], axis=0
        )

    started = []
    for copy in small:
        copy.wait()
    current = st_v[...].astype(F32)
    for l in range(layers):
        square = jnp.sum(current * current, axis=1, keepdims=True)
        normed = (current * gain_v[l:l + 1, :].astype(F32)).astype(BF16)
        wide = jnp.broadcast_to(square, (seqs, LANES))
        for d in range(n_dp):
            sq_s[l, d] = wide[d * local:(d + 1) * local]

        def send(src, dst, ss, rs, axis, index, size):
            for k in range(1, size):
                peer = lax.rem(index + k, size)
                copy = pltpu.make_async_remote_copy(
                    src_ref=src(peer), dst_ref=dst(index), send_sem=ss.at[k], recv_sem=rs.at[index],
                    device_id={axis: peer}, device_id_type=MESH,
                )
                copy.start()
                started.append(copy)

        def receive(src, dst, ss, rs, axis, index, size):
            for k in range(1, size):
                peer = lax.rem(index + k, size)
                pltpu.make_async_remote_copy(
                    src_ref=src(peer), dst_ref=dst(peer), send_sem=ss.at[k], recv_sem=rs.at[peer],
                    device_id={axis: peer}, device_id_type=MESH,
                ).wait_recv()

        sq_args = (
            lambda p: sq_s.at[l, p], lambda p: sq_r.at[l, p], sq_ss.at[l], sq_rs.at[l], "dp", dp, n_dp,
        )
        pj_args = [
            (
                lambda p, c=c: proj_s.at[l, c, p], lambda p, c=c: proj_r.at[l, c, p],
                pj_ss.at[l, c], pj_rs.at[l, c], "dp", dp, n_dp,
            )
            for c in range(PAIRS)
        ]
        for r in range(ROLES):
            w_copy[l][r].wait()
            value = jnp.dot(normed, w_v[l, r], preferred_element_type=F32)
            for d in range(n_dp):
                block = value[d * local:(d + 1) * local]
                proj_s[l, r // 2, d, r % 2] = jnp.concatenate(
                    [block[:, g * LANES:(g + 1) * LANES] for g in range(groups)], axis=0
                ).astype(BF16)
            if r % 2 == 1:
                if l == 0 and r == 1:
                    pl.semaphore_wait(barrier, n_dp - 1 + n_tp - 1)
                if r == 1:
                    send(*sq_args)
                send(*pj_args[r // 2])
        if l == 0:
            s_copy[0].start()
            ow_copy[0].start()
            for copy in w_copy[1]:
                copy.start()
            s_copy[1].start()
            ow_copy[1].start()

        s_copy[l].wait()
        for q in range(local):
            sb_v[l, q] = s_v[l, q].reshape(width, head).astype(BF16)

        receive(*sq_args)
        total = sq_s[l, dp]
        for k in range(1, n_dp):
            total = total + sq_r[l, lax.rem(dp + k, n_dp)]
        inv_rms = lax.rsqrt(total / width_all + 1e-06)
        inv_rms = jnp.concatenate([inv_rms] * groups, axis=0)

        roles = []
        for c in range(PAIRS):
            receive(*pj_args[c])
            for half in range(2):
                acc = proj_s[l, c, dp, half].astype(F32)
                for k in range(1, n_dp):
                    acc = acc + proj_r[l, c, lax.rem(dp + k, n_dp), half].astype(F32)
                roles.append(acc * inv_rms)
        key, recept, decay_pre, rate_pre, val, gate_pre = roles

        decay = jnp.exp(-0.606531 * jax.nn.sigmoid(fold(bias_v[l:l + 1, :]) + decay_pre))
        rate = jax.nn.sigmoid(rate_pre)
        vectors = split2(jnp.concatenate([key, decay * recept], axis=0))
        lhs = jnp.concatenate([vectors[:, :head], vectors[:, head:]], axis=0).astype(BF16)
        found = jnp.zeros((2 * rows, LANES), F32)
        for q in range(local):
            prod = lax.dot_general(lhs, sb_v[l, q], (((1,), (1,)), ((), ())), preferred_element_type=F32)
            first = prod[:2 * rows] + prod[2 * rows:4 * rows]
            second = prod[4 * rows:6 * rows] + prod[6 * rows:]
            for g in range(groups):
                at = g * local + q
                lanes = slice(g * LANES, (g + 1) * LANES)
                mine = (pair_row == at) | (pair_row == rows + at)
                found = jnp.where(mine, jnp.where(first_head, first[:, lanes], second[:, lanes]), found)

        sums = head_sum(jnp.concatenate([key * key, key * rate * recept, key * recept], axis=0))
        inv_norm = lax.rsqrt(sums[:rows] + 1e-06)
        removed = found[:rows] * inv_norm
        key_rate = key * rate * inv_norm
        read = found[rows:] - removed * (sums[rows:2 * rows] * inv_norm) + val * sums[2 * rows:]
        center = read - head_sum(read) / head
        normal = center * lax.rsqrt(head_sum(center * center) / head + 1e-05)
        mixed = normal * fold(hgain_v[l:l + 1, :].astype(F32)) * jax.nn.sigmoid(gate_pre)
        mix_s[l] = mixed.astype(BF16)
        mx_args = (lambda p: mix_s.at[l], lambda p: mix_r.at[l, p], mx_ss.at[l], mx_rs.at[l], "dp", dp, n_dp)
        send(*mx_args)
        mix_r[l, dp] = mix_s[l]

        tall = jnp.concatenate([removed, val, jnp.zeros((LANES - 2 * rows, LANES), F32)], axis=0)
        tall = jnp.transpose(tall)
        halves = [[x[:, half * head:(half + 1) * head] for x in (decay, key_rate, key)] for half in range(2)]
        for g in range(groups):
            for q in range(local):
                at = g * local + q
                for half in range(2):
                    h = 2 * g + half
                    d_row, r_row, k_row = [x[at:at + 1] for x in halves[half]]
                    part = tall[half * head:(half + 1) * head]
                    so_v[l, q, h] = (
                        s_v[l, q, h] * d_row - part[:, at:at + 1] * r_row + part[:, rows + at:rows + at + 1] * k_row
                    )
        so_copy = pltpu.make_async_copy(so_v.at[l], out_states.at[l], so_sem.at[l])
        so_copy.start()

        ow_copy[l].wait()
        receive(*mx_args)
        blocks = [mix_r[l, s].astype(F32) for s in range(n_dp)]
        gathered = jnp.concatenate(
            [
                jnp.concatenate([b[g * local:(g + 1) * local] for b in blocks], axis=0)
                for g in range(groups)
            ],
            axis=1,
        ).astype(BF16)
        br_s[l] = jnp.dot(gathered, ow_v[l], preferred_element_type=F32).astype(BF16)
        br_args = (lambda p: br_s.at[l], lambda p: br_r.at[l, p], br_ss.at[l], br_rs.at[l], "tp", tp, n_tp)
        send(*br_args)
        br_r[l, tp] = br_s[l]
        receive(*br_args)
        branch = br_r[l, 0].astype(F32)
        for s in range(1, n_tp):
            branch = branch + br_r[l, s].astype(F32)
        rounded = (current + branch).astype(BF16)
        current = rounded.astype(F32)
        if l == layers - 1:
            fin_v[...] = rounded
            fin = pltpu.make_async_copy(fin_v, out_stream, fin_sem)
            fin.start()
            fin.wait()

    for copy in started:
        copy.wait_send()
    for l in range(layers):
        pltpu.make_async_copy(so_v.at[l], out_states.at[l], so_sem.at[l]).wait()


def solution(mesh):
    n_dp, n_tp = mesh.shape["dp"], mesh.shape["tp"]

    def per_device(stream, states, gain, rw, kw, vw, dw, tw, gw, ow, bias, hgain):
        seqs, cols = stream.shape
        layers, local, heads, head, _ = states.shape
        width = heads * head
        rows = width // LANES * local
        dma = pltpu.SemaphoreType.DMA
        any_spec = pl.BlockSpec(memory_space=pl.ANY)
        return pl.pallas_call(
            functools.partial(kernel, n_dp, n_tp, cols * n_dp),
            out_shape=(
                jax.ShapeDtypeStruct(stream.shape, BF16),
                jax.ShapeDtypeStruct(states.shape, F32),
            ),
            in_specs=[any_spec] * 12,
            out_specs=(any_spec, any_spec),
            scratch_shapes=[
                pltpu.VMEM(stream.shape, BF16),
                pltpu.VMEM(states.shape, F32),
                pltpu.VMEM(states.shape, F32),
                pltpu.VMEM((layers, local, width, head), BF16),
                pltpu.VMEM(gain.shape, BF16),
                pltpu.VMEM((layers, ROLES, cols, width), BF16),
                pltpu.VMEM(ow.shape, BF16),
                pltpu.VMEM(bias.shape, F32),
                pltpu.VMEM(hgain.shape, BF16),
                pltpu.VMEM(stream.shape, BF16),
                pltpu.VMEM((layers, PAIRS, n_dp, 2, rows, LANES), BF16),
                pltpu.VMEM((layers, PAIRS, n_dp, 2, rows, LANES), BF16),
                pltpu.VMEM((layers, n_dp, local, LANES), F32),
                pltpu.VMEM((layers, n_dp, local, LANES), F32),
                pltpu.VMEM((layers, rows, LANES), BF16),
                pltpu.VMEM((layers, n_dp, rows, LANES), BF16),
                pltpu.VMEM((layers, seqs, cols), BF16),
                pltpu.VMEM((layers, n_tp, seqs, cols), BF16),
                dma((4,)),
                dma((layers, ROLES)),
                dma((layers,)),
                dma((layers,)),
                dma((layers,)),
                dma,
                dma((layers, PAIRS, n_dp)),
                dma((layers, PAIRS, n_dp)),
                dma((layers, n_dp)),
                dma((layers, n_dp)),
                dma((layers, n_dp)),
                dma((layers, n_dp)),
                dma((layers, n_tp)),
                dma((layers, n_tp)),
            ],
            compiler_params=pltpu.CompilerParams(
                collective_id=0, has_side_effects=True, vmem_limit_bytes=60 * 1024 * 1024
            ),
            name="two_blocks",
        )(stream, states, gain, rw, kw, vw, dw, tw, gw, ow, bias, hgain)

    in_specs = (
        P("grp", "dp"),
        P(None, ("grp", "dp"), "tp", None, None),
        P(None, "dp"),
        P(None, "dp", "tp"),
        P(None, "dp", "tp"),
        P(None, "dp", "tp"),
        P(None, "dp", "tp"),
        P(None, "dp", "tp"),
        P(None, "dp", "tp"),
        P(None, "tp", "dp"),
        P(None, "tp"),
        P(None, "tp"),
    )
    out_specs = (P("grp", "dp"), P(None, ("grp", "dp"), "tp", None, None))
    return jax.shard_map(
        per_device, mesh=mesh, in_specs=in_specs, out_specs=out_specs, check_vma=False
    )
```

```python
import functools

import jax
import jax.numpy as jnp
from jax import lax
from jax.experimental import pallas as pl
from jax.experimental.pallas import tpu as pltpu
from jax.sharding import PartitionSpec as P

F32 = jnp.float32
BF16 = jnp.bfloat16
MESH = pl.DeviceIdType.MESH
LANES = 128
ROLES = 6
KEY, RECEPT, DECAY, RATE, VALUE, GATE = range(ROLES)
PAIRS = ROLES // 2


def split2(x):
    high = x.astype(BF16).astype(F32)
    return jnp.concatenate([high, x - high], axis=0)


def kernel(
    n_dp, n_tp, width_all,
    stream, states, gain, rw, kw, vw, dw, tw, gw, ow, bias, hgain,
    out_stream, out_states,
    st_v, s_v, sb_v, gain_v, w_v, ow_v, bias_v, hgain_v,
    proj_s, proj_r, sq_s, sq_r, mix_s, mix_r, br_s, br_r,
    small_sem, w_sem, ow_sem, s_sem,
    pj_ss, pj_rs, sq_ss, sq_rs, mx_ss, mx_rs, br_ss, br_rs,
):
    dp = lax.axis_index("dp")
    tp = lax.axis_index("tp")
    seqs, cols = stream.shape
    layers, local, heads, head, _ = states.shape
    width = heads * head
    groups = width // LANES
    rows = groups * local

    small = [
        pltpu.make_async_copy(src, dst, small_sem.at[i])
        for i, (src, dst) in enumerate(
            [(stream, st_v), (gain, gain_v), (bias, bias_v), (hgain, hgain_v)]
        )
    ]
    weights = (kw, rw, dw, tw, vw, gw)
    w_copy = [
        [pltpu.make_async_copy(weights[r].at[l], w_v.at[l, r], w_sem.at[l, r]) for r in range(ROLES)]
        for l in range(layers)
    ]
    ow_copy = [pltpu.make_async_copy(ow.at[l], ow_v.at[l], ow_sem.at[l]) for l in range(layers)]
    s_copy = [pltpu.make_async_copy(states.at[l], s_v.at[l], s_sem.at[l]) for l in range(layers)]
    for copy in small:
        copy.start()
    for copy in w_copy[0]:
        copy.start()
    s_copy[0].start()

    barrier = pltpu.get_barrier_semaphore()
    for k in range(1, n_dp):
        pl.semaphore_signal(barrier, inc=1, device_id={"dp": lax.rem(dp + k, n_dp)}, device_id_type=MESH)
    for k in range(1, n_tp):
        pl.semaphore_signal(barrier, inc=1, device_id={"tp": lax.rem(tp + k, n_tp)}, device_id_type=MESH)

    lane_r = lax.broadcasted_iota(jnp.int32, (LANES, LANES), 0)
    lane_c = lax.broadcasted_iota(jnp.int32, (LANES, LANES), 1)
    same_head = jnp.where((lane_r < head) == (lane_c < head), 1.0, 0.0).astype(BF16)

    def head_sum(x):
        both = jnp.dot(split2(x).astype(BF16), same_head, preferred_element_type=F32)
        return both[: x.shape[0]] + both[x.shape[0]:]

    first_head = lax.broadcasted_iota(jnp.int32, (2 * rows, LANES), 1) < head
    pair_row = lax.broadcasted_iota(jnp.int32, (2 * rows, LANES), 0)

    def fold(row):
        return jnp.concatenate(
            [jnp.broadcast_to(row[:, g * LANES:(g + 1) * LANES], (local, LANES)) for g in range(groups)], axis=0
        )

    started = []
    for copy in small[:2]:
        copy.wait()
    current = st_v[...].astype(F32)
    for l in range(layers):
        square = jnp.sum(current * current, axis=1, keepdims=True)
        normed = (current * gain_v[l:l + 1, :].astype(F32)).astype(BF16)
        wide = jnp.broadcast_to(square, (seqs, LANES))
        for d in range(n_dp):
            sq_s[l, d] = wide[d * local:(d + 1) * local]

        def send(src, dst, ss, rs, axis, index, size):
            for k in range(1, size):
                peer = lax.rem(index + k, size)
                copy = pltpu.make_async_remote_copy(
                    src_ref=src(peer), dst_ref=dst(index), send_sem=ss.at[k], recv_sem=rs.at[index],
                    device_id={axis: peer}, device_id_type=MESH,
                )
                copy.start()
                started.append(copy)

        def receive(src, dst, ss, rs, axis, index, size):
            for k in range(1, size):
                peer = lax.rem(index + k, size)
                pltpu.make_async_remote_copy(
                    src_ref=src(peer), dst_ref=dst(peer), send_sem=ss.at[k], recv_sem=rs.at[peer],
                    device_id={axis: peer}, device_id_type=MESH,
                ).wait_recv()

        sq_args = (
            lambda p: sq_s.at[l, p], lambda p: sq_r.at[l, p], sq_ss.at[l], sq_rs.at[l], "dp", dp, n_dp,
        )
        pj_args = [
            (
                lambda p, c=c: proj_s.at[l, c, p], lambda p, c=c: proj_r.at[l, c, p],
                pj_ss.at[l, c], pj_rs.at[l, c], "dp", dp, n_dp,
            )
            for c in range(PAIRS)
        ]
        for r in range(ROLES):
            w_copy[l][r].wait()
            value = jnp.dot(normed, w_v[l, r], preferred_element_type=F32)
            for d in range(n_dp):
                block = value[d * local:(d + 1) * local]
                proj_s[l, r // 2, d, r % 2] = jnp.concatenate(
                    [block[:, g * LANES:(g + 1) * LANES] for g in range(groups)], axis=0
                ).astype(BF16)
            if l > 0 and r % 2 == 1:
                if r == 1:
                    send(*sq_args)
                send(*pj_args[r // 2])
        if l == 0:
            pl.semaphore_wait(barrier, n_dp - 1 + n_tp - 1)
            send(*sq_args)
            for c in range(PAIRS):
                send(*pj_args[c])
            for copy in small[2:]:
                copy.wait()
        s_copy[l].wait()
        for q in range(local):
            sb_v[l, q] = s_v[l, q].reshape(width, head).astype(BF16)
        if l == 0:
            ow_copy[0].start()
            for later in range(1, layers):
                for copy in w_copy[later]:
                    copy.start()
                s_copy[later].start()
                ow_copy[later].start()

        receive(*sq_args)
        total = sq_s[l, dp]
        for k in range(1, n_dp):
            total = total + sq_r[l, lax.rem(dp + k, n_dp)]
        inv_rms = lax.rsqrt(total / width_all + 1e-06)
        inv_rms = jnp.concatenate([inv_rms] * groups, axis=0)

        def projected(c):
            receive(*pj_args[c])
            for half in range(2):
                acc = proj_s[l, c, dp, half].astype(F32)
                for k in range(1, n_dp):
                    acc = acc + proj_r[l, c, lax.rem(dp + k, n_dp), half].astype(F32)
                yield acc * inv_rms

        key, recept = projected(0)
        decay_pre, rate_pre = projected(1)

        decay = jnp.exp(-0.606531 * jax.nn.sigmoid(fold(bias_v[l:l + 1, :]) + decay_pre))
        rate = jax.nn.sigmoid(rate_pre)
        vectors = split2(jnp.concatenate([key, decay * recept], axis=0))
        lhs = jnp.concatenate([vectors[:, :head], vectors[:, head:]], axis=0).astype(BF16)
        found = jnp.zeros((2 * rows, LANES), F32)
        for q in range(local):
            prod = lax.dot_general(lhs, sb_v[l, q], (((1,), (1,)), ((), ())), preferred_element_type=F32)
            first = prod[:2 * rows] + prod[2 * rows:4 * rows]
            second = prod[4 * rows:6 * rows] + prod[6 * rows:]
            for g in range(groups):
                at = g * local + q
                lanes = slice(g * LANES, (g + 1) * LANES)
                mine = (pair_row == at) | (pair_row == rows + at)
                found = jnp.where(mine, jnp.where(first_head, first[:, lanes], second[:, lanes]), found)

        sums = head_sum(jnp.concatenate([key * key, key * rate * recept, key * recept], axis=0))
        inv_norm = lax.rsqrt(sums[:rows] + 1e-06)
        removed = found[:rows] * inv_norm
        key_rate = key * rate * inv_norm
        val, gate_pre = projected(2)
        read = found[rows:] - removed * (sums[rows:2 * rows] * inv_norm) + val * sums[2 * rows:]
        center = read - head_sum(read) / head
        normal = center * lax.rsqrt(head_sum(center * center) / head + 1e-05)
        mixed = normal * fold(hgain_v[l:l + 1, :].astype(F32)) * jax.nn.sigmoid(gate_pre)
        mix_s[l] = mixed.astype(BF16)
        mx_args = (lambda p: mix_s.at[l], lambda p: mix_r.at[l, p], mx_ss.at[l], mx_rs.at[l], "dp", dp, n_dp)
        send(*mx_args)
        mix_r[l, dp] = mix_s[l]

        tall = jnp.concatenate([removed, val, jnp.zeros((LANES - 2 * rows, LANES), F32)], axis=0)
        tall = jnp.transpose(tall)
        halves = [[x[:, half * head:(half + 1) * head] for x in (decay, key_rate, key)] for half in range(2)]

        def renew(first_row, last_row):
            for at in range(first_row, last_row):
                g, q = at // local, at % local
                for half in range(2):
                    h = 2 * g + half
                    d_row, r_row, k_row = [x[at:at + 1] for x in halves[half]]
                    part = tall[half * head:(half + 1) * head]
                    out_states[l, q, h] = (
                        s_v[l, q, h] * d_row - part[:, at:at + 1] * r_row + part[:, rows + at:rows + at + 1] * k_row
                    )

        renew(0, rows // 2)

        ow_copy[l].wait()
        receive(*mx_args)
        blocks = [mix_r[l, s].astype(F32) for s in range(n_dp)]
        gathered = jnp.concatenate(
            [
                jnp.concatenate([b[g * local:(g + 1) * local] for b in blocks], axis=0)
                for g in range(groups)
            ],
            axis=1,
        ).astype(BF16)
        br_s[l] = jnp.dot(gathered, ow_v[l], preferred_element_type=F32).astype(BF16)
        br_args = (lambda p: br_s.at[l], lambda p: br_r.at[l, p], br_ss.at[l], br_rs.at[l], "tp", tp, n_tp)
        send(*br_args)
        br_r[l, tp] = br_s[l]
        renew(rows // 2, rows)
        receive(*br_args)
        branch = br_r[l, 0].astype(F32)
        for s in range(1, n_tp):
            branch = branch + br_r[l, s].astype(F32)
        rounded = (current + branch).astype(BF16)
        current = rounded.astype(F32)
        if l == layers - 1:
            out_stream[...] = rounded

    for copy in started:
        copy.wait_send()


def solution(mesh):
    n_dp, n_tp = mesh.shape["dp"], mesh.shape["tp"]

    def per_device(stream, states, gain, rw, kw, vw, dw, tw, gw, ow, bias, hgain):
        seqs, cols = stream.shape
        layers, local, heads, head, _ = states.shape
        width = heads * head
        rows = width // LANES * local
        dma = pltpu.SemaphoreType.DMA
        hbm_spec = pl.BlockSpec(memory_space=pltpu.HBM)
        return pl.pallas_call(
            functools.partial(kernel, n_dp, n_tp, cols * n_dp),
            out_shape=(
                pltpu.VMEM(stream.shape, BF16),
                pltpu.VMEM(states.shape, F32),
            ),
            in_specs=[hbm_spec] * 12,
            out_specs=(pl.BlockSpec(memory_space=pltpu.VMEM),) * 2,
            scratch_shapes=[
                pltpu.VMEM(stream.shape, BF16),
                pltpu.VMEM(states.shape, F32),
                pltpu.VMEM((layers, local, width, head), BF16),
                pltpu.VMEM(gain.shape, BF16),
                pltpu.VMEM((layers, ROLES, cols, width), BF16),
                pltpu.VMEM(ow.shape, BF16),
                pltpu.VMEM(bias.shape, F32),
                pltpu.VMEM(hgain.shape, BF16),
                pltpu.VMEM((layers, PAIRS, n_dp, 2, rows, LANES), BF16),
                pltpu.VMEM((layers, PAIRS, n_dp, 2, rows, LANES), BF16),
                pltpu.VMEM((layers, n_dp, local, LANES), F32),
                pltpu.VMEM((layers, n_dp, local, LANES), F32),
                pltpu.VMEM((layers, rows, LANES), BF16),
                pltpu.VMEM((layers, n_dp, rows, LANES), BF16),
                pltpu.VMEM((layers, seqs, cols), BF16),
                pltpu.VMEM((layers, n_tp, seqs, cols), BF16),
                dma((4,)),
                dma((layers, ROLES)),
                dma((layers,)),
                dma((layers,)),
                dma((layers, PAIRS, n_dp)),
                dma((layers, PAIRS, n_dp)),
                dma((layers, n_dp)),
                dma((layers, n_dp)),
                dma((layers, n_dp)),
                dma((layers, n_dp)),
                dma((layers, n_tp)),
                dma((layers, n_tp)),
            ],
            compiler_params=pltpu.CompilerParams(
                collective_id=0, has_side_effects=True, vmem_limit_bytes=56 * 1024 * 1024
            ),
            name="two_blocks",
        )(stream, states, gain, rw, kw, vw, dw, tw, gw, ow, bias, hgain)

    in_specs = (
        P("grp", "dp"),
        P(None, ("grp", "dp"), "tp", None, None),
        P(None, "dp"),
        P(None, "dp", "tp"),
        P(None, "dp", "tp"),
        P(None, "dp", "tp"),
        P(None, "dp", "tp"),
        P(None, "dp", "tp"),
        P(None, "dp", "tp"),
        P(None, "tp", "dp"),
        P(None, "tp"),
        P(None, "tp"),
    )
    out_specs = (P("grp", "dp"), P(None, ("grp", "dp"), "tp", None, None))
    return jax.shard_map(
        per_device, mesh=mesh, in_specs=in_specs, out_specs=out_specs, check_vma=False
    )
```

```python
import functools

import jax
import jax.numpy as jnp
from jax import lax
from jax.experimental import pallas as pl
from jax.experimental.pallas import tpu as pltpu
from jax.sharding import PartitionSpec as P

F32 = jnp.float32
BF16 = jnp.bfloat16
MESH = pl.DeviceIdType.MESH
LANES = 128
ROLES = 6
KEY, RECEPT, DECAY, RATE, VALUE, GATE = range(ROLES)
PAIRS = ROLES // 2


def split2(x):
    high = x.astype(BF16).astype(F32)
    return jnp.concatenate([high, x - high], axis=0)


def kernel(
    n_dp, n_tp, width_all,
    stream, states, gain, rw, kw, vw, dw, tw, gw, ow, bias, hgain,
    out_stream, out_states,
    st_v, s_v, sb_v, gain_v, w_v, ow_v, bias_v, hgain_v,
    proj_s, proj_r, sq_s, sq_r, mix_s, mix_r, br_s, br_r,
    small_sem, w_sem, ow_sem, s_sem,
    pj_ss, pj_rs, sq_ss, sq_rs, mx_ss, mx_rs, br_ss, br_rs,
):
    dp = lax.axis_index("dp")
    tp = lax.axis_index("tp")
    seqs, cols = stream.shape
    layers, local, heads, head, _ = states.shape
    width = heads * head
    groups = width // LANES
    rows = groups * local

    small = [
        pltpu.make_async_copy(src, dst, small_sem.at[i])
        for i, (src, dst) in enumerate(
            [(stream, st_v), (gain, gain_v), (bias, bias_v), (hgain, hgain_v)]
        )
    ]
    weights = (kw, rw, dw, tw, vw, gw)
    w_copy = [
        [pltpu.make_async_copy(weights[r].at[l], w_v.at[l, r], w_sem.at[l, r]) for r in range(ROLES)]
        for l in range(layers)
    ]
    ow_copy = [pltpu.make_async_copy(ow.at[l], ow_v.at[l], ow_sem.at[l]) for l in range(layers)]
    s_copy = [pltpu.make_async_copy(states.at[l], s_v.at[l], s_sem.at[l]) for l in range(layers)]
    for copy in small:
        copy.start()
    for copy in w_copy[0]:
        copy.start()
    s_copy[0].start()

    barrier = pltpu.get_barrier_semaphore()
    for k in range(1, n_dp):
        pl.semaphore_signal(barrier, inc=1, device_id={"dp": lax.rem(dp + k, n_dp)}, device_id_type=MESH)
    for k in range(1, n_tp):
        pl.semaphore_signal(barrier, inc=1, device_id={"tp": lax.rem(tp + k, n_tp)}, device_id_type=MESH)

    lane_r = lax.broadcasted_iota(jnp.int32, (LANES, LANES), 0)
    lane_c = lax.broadcasted_iota(jnp.int32, (LANES, LANES), 1)
    same_head = jnp.where((lane_r < head) == (lane_c < head), 1.0, 0.0).astype(BF16)

    def head_sum(x):
        both = jnp.dot(split2(x).astype(BF16), same_head, preferred_element_type=F32)
        return both[: x.shape[0]] + both[x.shape[0]:]

    first_head = lax.broadcasted_iota(jnp.int32, (2 * rows, LANES), 1) < head
    pair_row = lax.broadcasted_iota(jnp.int32, (2 * rows, LANES), 0)

    def fold(row):
        return jnp.concatenate(
            [jnp.broadcast_to(row[:, g * LANES:(g + 1) * LANES], (local, LANES)) for g in range(groups)], axis=0
        )

    started = []
    for copy in small[:2]:
        copy.wait()
    chunks = br_s.shape[1]
    part_cols = cols // chunks
    spans = [slice(c * part_cols, (c + 1) * part_cols) for c in range(chunks)]
    current = [st_v[:, span].astype(F32) for span in spans]
    for l in range(layers):

        def norm(c):
            x = current[c]
            square = jnp.sum(x * x, axis=1, keepdims=True)
            return square, (x * gain_v[l:l + 1, spans[c]].astype(F32)).astype(BF16)

        def send(src, dst, ss, rs, axis, index, size):
            for k in range(1, size):
                peer = lax.rem(index + k, size)
                if axis == "tp":
                    down, up = size - k, k - 1
                    down = jnp.where(down > index, down, down - 1)
                    up = jnp.where(up < index, up, up + 1)
                    peer = jnp.where(2 * index < size, down, up)
                copy = pltpu.make_async_remote_copy(
                    src_ref=src(peer), dst_ref=dst(index), send_sem=ss.at[k], recv_sem=rs.at[index],
                    device_id={axis: peer}, device_id_type=MESH,
                )
                copy.start()
                started.append(copy)

        def receive(src, dst, ss, rs, axis, index, size):
            for k in range(1, size):
                peer = lax.rem(index + k, size)
                pltpu.make_async_remote_copy(
                    src_ref=src(peer), dst_ref=dst(peer), send_sem=ss.at[k], recv_sem=rs.at[peer],
                    device_id={axis: peer}, device_id_type=MESH,
                ).wait_recv()

        sq_args = (
            lambda p: sq_s.at[l, p], lambda p: sq_r.at[l, p], sq_ss.at[l], sq_rs.at[l], "dp", dp, n_dp,
        )
        pj_args = [
            (
                lambda p, c=c: proj_s.at[l, c, p], lambda p, c=c: proj_r.at[l, c, p],
                pj_ss.at[l, c], pj_rs.at[l, c], "dp", dp, n_dp,
            )
            for c in range(PAIRS)
        ]
        parts = []
        if l == 0:
            squares, normed = zip(*[norm(c) for c in range(chunks)])
            square, last = sum(squares), jnp.concatenate(normed, axis=1)
            last_span = slice(0, cols)
        else:
            square = 0.0
            for c in range(chunks):
                current[c] = arrive(c)
                more, last = norm(c)
                square = square + more
                last_span = spans[c]
                if c < chunks - 1:
                    for r in range(ROLES):
                        if c == 0:
                            w_copy[l][r].wait()
                        value = jnp.dot(last, w_v[l, r, last_span], preferred_element_type=F32)
                        if c == 0:
                            parts.append(value)
                        else:
                            parts[r] = parts[r] + value
        wide = jnp.broadcast_to(square, (seqs, LANES))
        for d in range(n_dp):
            sq_s[l, d] = wide[d * local:(d + 1) * local]
        if l > 0:
            send(*sq_args)
        for r in range(ROLES):
            if not parts:
                w_copy[l][r].wait()
            value = jnp.dot(last, w_v[l, r, last_span], preferred_element_type=F32)
            if parts:
                value = value + parts[r]
            for d in range(n_dp):
                block = value[d * local:(d + 1) * local]
                proj_s[l, r // 2, d, r % 2] = jnp.concatenate(
                    [block[:, g * LANES:(g + 1) * LANES] for g in range(groups)], axis=0
                ).astype(BF16)
            if l == 0 and r == 3:
                pl.semaphore_wait(barrier, n_dp - 1 + n_tp - 1)
                send(*sq_args)
                send(*pj_args[0])
            if r % 2 == 1 and (l > 0 or r > 1):
                send(*pj_args[r // 2])
        if l == 0:
            for copy in small[2:]:
                copy.wait()
        s_copy[l].wait()
        for q in range(local):
            sb_v[l, q] = s_v[l, q].reshape(width, head).astype(BF16)
        if l == 0:
            ow_copy[0].start()
            for later in range(1, layers):
                for copy in w_copy[later]:
                    copy.start()
                s_copy[later].start()
                ow_copy[later].start()

        receive(*sq_args)
        total = sq_s[l, dp]
        for k in range(1, n_dp):
            total = total + sq_r[l, lax.rem(dp + k, n_dp)]
        inv_rms = lax.rsqrt(total / width_all + 1e-06)
        inv_rms = jnp.concatenate([inv_rms] * groups, axis=0)

        def projected(c):
            receive(*pj_args[c])
            for half in range(2):
                acc = proj_s[l, c, dp, half].astype(F32)
                for k in range(1, n_dp):
                    acc = acc + proj_r[l, c, lax.rem(dp + k, n_dp), half].astype(F32)
                yield acc * inv_rms

        key, recept = projected(0)
        decay_pre, rate_pre = projected(1)

        decay = jnp.exp(-0.606531 * jax.nn.sigmoid(fold(bias_v[l:l + 1, :]) + decay_pre))
        rate = jax.nn.sigmoid(rate_pre)
        vectors = split2(jnp.concatenate([key, decay * recept], axis=0))
        lhs = jnp.concatenate([vectors[:, :head], vectors[:, head:]], axis=0).astype(BF16)
        found = jnp.zeros((2 * rows, LANES), F32)
        for q in range(local):
            prod = lax.dot_general(lhs, sb_v[l, q], (((1,), (1,)), ((), ())), preferred_element_type=F32)
            first = prod[:2 * rows] + prod[2 * rows:4 * rows]
            second = prod[4 * rows:6 * rows] + prod[6 * rows:]
            for g in range(groups):
                at = g * local + q
                lanes = slice(g * LANES, (g + 1) * LANES)
                mine = (pair_row == at) | (pair_row == rows + at)
                found = jnp.where(mine, jnp.where(first_head, first[:, lanes], second[:, lanes]), found)

        sums = head_sum(jnp.concatenate([key * key, key * rate * recept, key * recept], axis=0))
        inv_norm = lax.rsqrt(sums[:rows] + 1e-06)
        removed = found[:rows] * inv_norm
        key_rate = key * rate * inv_norm
        val, gate_pre = projected(2)
        read = found[rows:] - removed * (sums[rows:2 * rows] * inv_norm) + val * sums[2 * rows:]
        center = read - head_sum(read) / head
        normal = center * lax.rsqrt(head_sum(center * center) / head + 1e-05)
        mixed = normal * fold(hgain_v[l:l + 1, :].astype(F32)) * jax.nn.sigmoid(gate_pre)
        mix_s[l] = mixed.astype(BF16)
        mx_args = (lambda p: mix_s.at[l], lambda p: mix_r.at[l, p], mx_ss.at[l], mx_rs.at[l], "dp", dp, n_dp)
        send(*mx_args)
        mix_r[l, dp] = mix_s[l]

        tall = jnp.concatenate([removed, val, jnp.zeros((LANES - 2 * rows, LANES), F32)], axis=0)
        tall = jnp.transpose(tall)
        halves = [[x[:, half * head:(half + 1) * head] for x in (decay, key_rate, key)] for half in range(2)]

        def renew(first_row, last_row):
            for at in range(first_row, last_row):
                g, q = at // local, at % local
                for half in range(2):
                    h = 2 * g + half
                    d_row, r_row, k_row = [x[at:at + 1] for x in halves[half]]
                    part = tall[half * head:(half + 1) * head]
                    out_states[l, q, h] = (
                        s_v[l, q, h] * d_row - part[:, at:at + 1] * r_row + part[:, rows + at:rows + at + 1] * k_row
                    )

        renew(0, rows // 2)

        ow_copy[l].wait()
        receive(*mx_args)
        blocks = [mix_r[l, s].astype(F32) for s in range(n_dp)]
        gathered = jnp.concatenate(
            [
                jnp.concatenate([b[g * local:(g + 1) * local] for b in blocks], axis=0)
                for g in range(groups)
            ],
            axis=1,
        ).astype(BF16)
        br_args = [
            (
                lambda p, c=c: br_s.at[l, c], lambda p, c=c: br_r.at[l, p, c],
                br_ss.at[l, c], br_rs.at[l, c], "tp", tp, n_tp,
            )
            for c in range(chunks)
        ]
        for c in range(chunks):
            br_s[l, c] = jnp.dot(gathered, ow_v[l, :, spans[c]], preferred_element_type=F32).astype(BF16)
            send(*br_args[c])
        for c in range(chunks):
            br_r[l, tp, c] = br_s[l, c]
        renew(rows // 2, rows)

        def arrive(c, l=l, receive=receive, br_args=br_args):
            receive(*br_args[c])
            branch = br_r[l, 0, c].astype(F32)
            for s in range(1, n_tp):
                branch = branch + br_r[l, s, c].astype(F32)
            return (current[c] + branch).astype(BF16).astype(F32)

    for c in range(chunks):
        out_stream[:, spans[c]] = arrive(c).astype(BF16)
    for copy in started:
        copy.wait_send()


def flush(stream, states, out_stream, out_states, sem):
    copies = [pltpu.make_async_copy(stream, out_stream, sem.at[0])]
    layers, local = states.shape[:2]
    for l in range(layers):
        for q in range(local):
            copies.append(
                pltpu.make_async_copy(states.at[l, q], out_states.at[l, q], sem.at[1 + l * local + q])
            )
    for copy in copies:
        copy.start()
    for copy in copies:
        copy.wait()


def solution(mesh):
    n_dp, n_tp = mesh.shape["dp"], mesh.shape["tp"]

    def per_device(stream, states, gain, rw, kw, vw, dw, tw, gw, ow, bias, hgain):
        seqs, cols = stream.shape
        layers, local, heads, head, _ = states.shape
        width = heads * head
        rows = width // LANES * local
        chunks = 2 if cols % (2 * LANES) == 0 else 1
        dma = pltpu.SemaphoreType.DMA
        hbm_spec = pl.BlockSpec(memory_space=pltpu.HBM)
        new_stream, new_states = pl.pallas_call(
            functools.partial(kernel, n_dp, n_tp, cols * n_dp),
            out_shape=(
                pltpu.VMEM(stream.shape, BF16),
                pltpu.VMEM(states.shape, F32),
            ),
            in_specs=[hbm_spec] * 12,
            out_specs=(pl.BlockSpec(memory_space=pltpu.VMEM),) * 2,
            scratch_shapes=[
                pltpu.VMEM(stream.shape, BF16),
                pltpu.VMEM(states.shape, F32),
                pltpu.VMEM((layers, local, width, head), BF16),
                pltpu.VMEM(gain.shape, BF16),
                pltpu.VMEM((layers, ROLES, cols, width), BF16),
                pltpu.VMEM(ow.shape, BF16),
                pltpu.VMEM(bias.shape, F32),
                pltpu.VMEM(hgain.shape, BF16),
                pltpu.VMEM((layers, PAIRS, n_dp, 2, rows, LANES), BF16),
                pltpu.VMEM((layers, PAIRS, n_dp, 2, rows, LANES), BF16),
                pltpu.VMEM((layers, n_dp, local, LANES), F32),
                pltpu.VMEM((layers, n_dp, local, LANES), F32),
                pltpu.VMEM((layers, rows, LANES), BF16),
                pltpu.VMEM((layers, n_dp, rows, LANES), BF16),
                pltpu.VMEM((layers, chunks, seqs, cols // chunks), BF16),
                pltpu.VMEM((layers, n_tp, chunks, seqs, cols // chunks), BF16),
                dma((4,)),
                dma((layers, ROLES)),
                dma((layers,)),
                dma((layers,)),
                dma((layers, PAIRS, n_dp)),
                dma((layers, PAIRS, n_dp)),
                dma((layers, n_dp)),
                dma((layers, n_dp)),
                dma((layers, n_dp)),
                dma((layers, n_dp)),
                dma((layers, chunks, n_tp)),
                dma((layers, chunks, n_tp)),
            ],
            compiler_params=pltpu.CompilerParams(
                collective_id=0, has_side_effects=True, vmem_limit_bytes=56 * 1024 * 1024
            ),
            name="two_blocks",
        )(stream, states, gain, rw, kw, vw, dw, tw, gw, ow, bias, hgain)
        return pl.pallas_call(
            flush,
            out_shape=(
                jax.ShapeDtypeStruct(stream.shape, BF16),
                jax.ShapeDtypeStruct(states.shape, F32),
            ),
            in_specs=[pl.BlockSpec(memory_space=pltpu.VMEM)] * 2,
            out_specs=(hbm_spec,) * 2,
            scratch_shapes=[dma((1 + layers * local,))],
            compiler_params=pltpu.CompilerParams(vmem_limit_bytes=1024 * 1024),
            name="flush",
        )(new_stream, new_states)

    in_specs = (
        P("grp", "dp"),
        P(None, ("grp", "dp"), "tp", None, None),
        P(None, "dp"),
        P(None, "dp", "tp"),
        P(None, "dp", "tp"),
        P(None, "dp", "tp"),
        P(None, "dp", "tp"),
        P(None, "dp", "tp"),
        P(None, "dp", "tp"),
        P(None, "tp", "dp"),
        P(None, "tp"),
        P(None, "tp"),
    )
    out_specs = (P("grp", "dp"), P(None, ("grp", "dp"), "tp", None, None))
    return jax.shard_map(
        per_device, mesh=mesh, in_specs=in_specs, out_specs=out_specs, check_vma=False
    )
```

```python
import functools

import jax
import jax.numpy as jnp
from jax import lax
from jax.experimental import pallas as pl
from jax.experimental.pallas import tpu as pltpu
from jax.sharding import PartitionSpec as P

F32 = jnp.float32
BF16 = jnp.bfloat16
MESH = pl.DeviceIdType.MESH
LANES = 128
ROLES = 6
KEY, RECEPT, DECAY, RATE, VALUE, GATE = range(ROLES)
PAIRS = ROLES // 2


def split2(x):
    high = x.astype(BF16).astype(F32)
    return jnp.concatenate([high, x - high], axis=0)


def kernel(
    n_dp, n_tp, width_all,
    stream, states, gain, rw, kw, vw, dw, tw, gw, ow, bias, hgain,
    out_stream, out_states,
    st_v, s_v, sb_v, gain_v, w_v, ow_v, bias_v, hgain_v,
    proj_s, proj_r, sq_s, sq_r, mix_s, mix_r, br_s, br_r,
    small_sem, w_sem, ow_sem, s_sem,
    pj_ss, pj_rs, sq_ss, sq_rs, mx_ss, mx_rs, br_ss, br_rs,
):
    dp = lax.axis_index("dp")
    tp = lax.axis_index("tp")
    seqs, cols = stream.shape
    layers, local, heads, head, _ = states.shape
    width = heads * head
    groups = width // LANES
    rows = groups * local

    small = [
        pltpu.make_async_copy(src, dst, small_sem.at[i])
        for i, (src, dst) in enumerate(
            [(stream, st_v), (gain, gain_v), (bias, bias_v), (hgain, hgain_v)]
        )
    ]
    weights = (kw, rw, dw, tw, vw, gw)
    w_copy = [
        [pltpu.make_async_copy(weights[r].at[l], w_v.at[l, r], w_sem.at[r]) for r in range(ROLES)]
        for l in range(layers)
    ]
    ow_copy = [pltpu.make_async_copy(ow.at[l], ow_v.at[l], ow_sem) for l in range(layers)]
    s_copy = [pltpu.make_async_copy(states.at[l], s_v.at[l], s_sem) for l in range(layers)]
    for copy in small:
        copy.start()
    for copy in w_copy[0]:
        copy.start()
    s_copy[0].start()

    barrier = pltpu.get_barrier_semaphore()
    for k in range(1, n_dp):
        pl.semaphore_signal(barrier, inc=1, device_id={"dp": lax.rem(dp + k, n_dp)}, device_id_type=MESH)
    for k in range(1, n_tp):
        pl.semaphore_signal(barrier, inc=1, device_id={"tp": lax.rem(tp + k, n_tp)}, device_id_type=MESH)

    lane_r = lax.broadcasted_iota(jnp.int32, (LANES, LANES), 0)
    lane_c = lax.broadcasted_iota(jnp.int32, (LANES, LANES), 1)
    same_head = jnp.where((lane_r < head) == (lane_c < head), 1.0, 0.0).astype(BF16)

    def head_sum(x):
        both = jnp.dot(split2(x).astype(BF16), same_head, preferred_element_type=F32)
        return both[: x.shape[0]] + both[x.shape[0]:]

    first_head = lax.broadcasted_iota(jnp.int32, (2 * rows, LANES), 1) < head
    pair_row = lax.broadcasted_iota(jnp.int32, (2 * rows, LANES), 0)

    def fold(row):
        return jnp.concatenate(
            [jnp.broadcast_to(row[:, g * LANES:(g + 1) * LANES], (local, LANES)) for g in range(groups)], axis=0
        )

    sent = []
    for copy in small[:2]:
        copy.wait()
    chunks = br_s.shape[1]
    part_cols = cols // chunks
    spans = [slice(c * part_cols, (c + 1) * part_cols) for c in range(chunks)]
    current = [st_v[:, span].astype(F32) for span in spans]
    for l in range(layers):

        def norm(c):
            x = current[c]
            square = jnp.sum(x * x, axis=1, keepdims=True)
            return square, (x * gain_v[l:l + 1, spans[c]].astype(F32)).astype(BF16)

        def send(src, dst, ss, rs, axis, index, size):
            for k in range(1, size):
                peer = lax.rem(index + k, size)
                slot = k - 1
                if axis == "tp":
                    down, up = size - k, k - 1
                    down = jnp.where(down > index, down, down - 1)
                    up = jnp.where(up < index, up, up + 1)
                    peer = jnp.where(2 * index < size, down, up)
                    slot = lax.rem(peer - index + size, size) - 1
                copy = pltpu.make_async_remote_copy(
                    src_ref=src(peer), dst_ref=dst(index), send_sem=ss.at[k - 1], recv_sem=rs.at[slot],
                    device_id={axis: peer}, device_id_type=MESH,
                )
                copy.start()
                sent.append(copy)

        def receive(src, dst, ss, rs, axis, index, size):
            for k in range(1, size):
                peer = lax.rem(index - k + size, size)
                pltpu.make_async_remote_copy(
                    src_ref=src(peer), dst_ref=dst(peer), send_sem=ss.at[k - 1], recv_sem=rs.at[k - 1],
                    device_id={axis: peer}, device_id_type=MESH,
                ).wait_recv()

        sq_args = (
            lambda p: sq_s.at[l, p], lambda p: sq_r.at[l, p], sq_ss, sq_rs, "dp", dp, n_dp,
        )
        pj_args = [
            (
                lambda p, c=c: proj_s.at[l, c, p], lambda p, c=c: proj_r.at[l, c, p],
                pj_ss.at[c], pj_rs.at[c], "dp", dp, n_dp,
            )
            for c in range(PAIRS)
        ]
        parts = []
        if l == 0:
            squares, normed = zip(*[norm(c) for c in range(chunks)])
            square, last = sum(squares), jnp.concatenate(normed, axis=1)
            last_span = slice(0, cols)
        else:
            square = 0.0
            for c in range(chunks):
                current[c] = arrive(c)
                more, last = norm(c)
                square = square + more
                last_span = spans[c]
                if c < chunks - 1:
                    for r in range(ROLES):
                        if c == 0:
                            w_copy[l][r].wait()
                        value = jnp.dot(last, w_v[l, r, last_span], preferred_element_type=F32)
                        if c == 0:
                            parts.append(value)
                        else:
                            parts[r] = parts[r] + value
        for copy in sent:
            copy.wait_send()
        sent.clear()
        wide = jnp.broadcast_to(square, (seqs, LANES))
        for d in range(n_dp):
            sq_s[l, d] = wide[d * local:(d + 1) * local]
        if l > 0:
            send(*sq_args)
        for r in range(ROLES):
            if not parts:
                w_copy[l][r].wait()
            value = jnp.dot(last, w_v[l, r, last_span], preferred_element_type=F32)
            if parts:
                value = value + parts[r]
            for d in range(n_dp):
                block = value[d * local:(d + 1) * local]
                proj_s[l, r // 2, d, r % 2] = jnp.concatenate(
                    [block[:, g * LANES:(g + 1) * LANES] for g in range(groups)], axis=0
                ).astype(BF16)
            if l == 0 and r == 3:
                pl.semaphore_wait(barrier, n_dp - 1 + n_tp - 1)
                send(*sq_args)
                send(*pj_args[0])
            if r % 2 == 1 and (l > 0 or r > 1):
                send(*pj_args[r // 2])
        if l == 0:
            for copy in small[2:]:
                copy.wait()
        s_copy[l].wait()
        for q in range(local):
            sb_v[l, q] = s_v[l, q].reshape(width, head).astype(BF16)
        if l == 0:
            ow_copy[0].start()
            for later in range(1, layers):
                for copy in w_copy[later]:
                    copy.start()
                s_copy[later].start()

        receive(*sq_args)
        total = sq_s[l, dp]
        for k in range(1, n_dp):
            total = total + sq_r[l, lax.rem(dp + k, n_dp)]
        inv_rms = lax.rsqrt(total / width_all + 1e-06)
        inv_rms = jnp.concatenate([inv_rms] * groups, axis=0)

        def projected(c):
            receive(*pj_args[c])
            for half in range(2):
                acc = proj_s[l, c, dp, half].astype(F32)
                for k in range(1, n_dp):
                    acc = acc + proj_r[l, c, lax.rem(dp + k, n_dp), half].astype(F32)
                yield acc * inv_rms

        key, recept = projected(0)
        decay_pre, rate_pre = projected(1)

        decay = jnp.exp(-0.606531 * jax.nn.sigmoid(fold(bias_v[l:l + 1, :]) + decay_pre))
        rate = jax.nn.sigmoid(rate_pre)
        vectors = split2(jnp.concatenate([key, decay * recept], axis=0))
        lhs = jnp.concatenate([vectors[:, :head], vectors[:, head:]], axis=0).astype(BF16)
        found = jnp.zeros((2 * rows, LANES), F32)
        for q in range(local):
            prod = lax.dot_general(lhs, sb_v[l, q], (((1,), (1,)), ((), ())), preferred_element_type=F32)
            first = prod[:2 * rows] + prod[2 * rows:4 * rows]
            second = prod[4 * rows:6 * rows] + prod[6 * rows:]
            for g in range(groups):
                at = g * local + q
                lanes = slice(g * LANES, (g + 1) * LANES)
                mine = (pair_row == at) | (pair_row == rows + at)
                found = jnp.where(mine, jnp.where(first_head, first[:, lanes], second[:, lanes]), found)

        sums = head_sum(jnp.concatenate([key * key, key * rate * recept, key * recept], axis=0))
        inv_norm = lax.rsqrt(sums[:rows] + 1e-06)
        removed = found[:rows] * inv_norm
        key_rate = key * rate * inv_norm
        val, gate_pre = projected(2)
        read = found[rows:] - removed * (sums[rows:2 * rows] * inv_norm) + val * sums[2 * rows:]
        center = read - head_sum(read) / head
        normal = center * lax.rsqrt(head_sum(center * center) / head + 1e-05)
        mixed = normal * fold(hgain_v[l:l + 1, :].astype(F32)) * jax.nn.sigmoid(gate_pre)
        mix_s[l] = mixed.astype(BF16)
        mx_args = (lambda p: mix_s.at[l], lambda p: mix_r.at[l, p], mx_ss, mx_rs, "dp", dp, n_dp)
        send(*mx_args)
        mix_r[l, dp] = mix_s[l]

        tall = jnp.concatenate([removed, val, jnp.zeros((LANES - 2 * rows, LANES), F32)], axis=0)
        tall = jnp.transpose(tall)
        halves = [[x[:, half * head:(half + 1) * head] for x in (decay, key_rate, key)] for half in range(2)]

        def renew(first_row, last_row):
            for at in range(first_row, last_row):
                g, q = at // local, at % local
                for half in range(2):
                    h = 2 * g + half
                    d_row, r_row, k_row = [x[at:at + 1] for x in halves[half]]
                    part = tall[half * head:(half + 1) * head]
                    out_states[l, q, h] = (
                        s_v[l, q, h] * d_row - part[:, at:at + 1] * r_row + part[:, rows + at:rows + at + 1] * k_row
                    )

        renew(0, rows // 2)

        ow_copy[l].wait()
        if l < layers - 1:
            ow_copy[l + 1].start()
        receive(*mx_args)
        blocks = [mix_r[l, s].astype(F32) for s in range(n_dp)]
        gathered = jnp.concatenate(
            [
                jnp.concatenate([b[g * local:(g + 1) * local] for b in blocks], axis=0)
                for g in range(groups)
            ],
            axis=1,
        ).astype(BF16)
        br_args = [
            (
                lambda p, c=c: br_s.at[l, c], lambda p, c=c: br_r.at[l, p, c],
                br_ss.at[c], br_rs.at[l, c], "tp", tp, n_tp,
            )
            for c in range(chunks)
        ]
        for c in range(chunks):
            br_s[l, c] = jnp.dot(gathered, ow_v[l, :, spans[c]], preferred_element_type=F32).astype(BF16)
            send(*br_args[c])
        for c in range(chunks):
            br_r[l, tp, c] = br_s[l, c]
        renew(rows // 2, rows)

        def arrive(c, l=l, receive=receive, br_args=br_args):
            receive(*br_args[c])
            branch = br_r[l, 0, c].astype(F32)
            for s in range(1, n_tp):
                branch = branch + br_r[l, s, c].astype(F32)
            return (current[c] + branch).astype(BF16).astype(F32)

    for c in range(chunks):
        out_stream[:, spans[c]] = arrive(c).astype(BF16)
    for copy in sent:
        copy.wait_send()


def flush(stream, states, out_stream, out_states, sem):
    copies = [pltpu.make_async_copy(stream, out_stream, sem.at[0])]
    for l in range(states.shape[0]):
        copies.append(pltpu.make_async_copy(states.at[l], out_states.at[l], sem.at[1 + l]))
    for copy in copies:
        copy.start()
    for copy in copies:
        copy.wait()


def solution(mesh):
    n_dp, n_tp = mesh.shape["dp"], mesh.shape["tp"]

    def per_device(stream, states, gain, rw, kw, vw, dw, tw, gw, ow, bias, hgain):
        seqs, cols = stream.shape
        layers, local, heads, head, _ = states.shape
        width = heads * head
        rows = width // LANES * local
        chunks = 2 if cols % (2 * LANES) == 0 else 1
        dma = pltpu.SemaphoreType.DMA
        hbm_spec = pl.BlockSpec(memory_space=pltpu.HBM)
        new_stream, new_states = pl.pallas_call(
            functools.partial(kernel, n_dp, n_tp, cols * n_dp),
            out_shape=(
                pltpu.VMEM(stream.shape, BF16),
                pltpu.VMEM(states.shape, F32),
            ),
            in_specs=[hbm_spec] * 12,
            out_specs=(pl.BlockSpec(memory_space=pltpu.VMEM),) * 2,
            scratch_shapes=[
                pltpu.VMEM(stream.shape, BF16),
                pltpu.VMEM(states.shape, F32),
                pltpu.VMEM((layers, local, width, head), BF16),
                pltpu.VMEM(gain.shape, BF16),
                pltpu.VMEM((layers, ROLES, cols, width), BF16),
                pltpu.VMEM(ow.shape, BF16),
                pltpu.VMEM(bias.shape, F32),
                pltpu.VMEM(hgain.shape, BF16),
                pltpu.VMEM((layers, PAIRS, n_dp, 2, rows, LANES), BF16),
                pltpu.VMEM((layers, PAIRS, n_dp, 2, rows, LANES), BF16),
                pltpu.VMEM((layers, n_dp, local, LANES), F32),
                pltpu.VMEM((layers, n_dp, local, LANES), F32),
                pltpu.VMEM((layers, rows, LANES), BF16),
                pltpu.VMEM((layers, n_dp, rows, LANES), BF16),
                pltpu.VMEM((layers, chunks, seqs, cols // chunks), BF16),
                pltpu.VMEM((layers, n_tp, chunks, seqs, cols // chunks), BF16),
                dma((4,)),
                dma((ROLES,)),
                dma,
                dma,
                dma((PAIRS, n_dp - 1)),
                dma((PAIRS, n_dp - 1)),
                dma((n_dp - 1,)),
                dma((n_dp - 1,)),
                dma((n_dp - 1,)),
                dma((n_dp - 1,)),
                dma((chunks, n_tp - 1)),
                dma((layers, chunks, n_tp - 1)),
            ],
            compiler_params=pltpu.CompilerParams(
                collective_id=0, has_side_effects=True, vmem_limit_bytes=56 * 1024 * 1024
            ),
            name="two_blocks",
        )(stream, states, gain, rw, kw, vw, dw, tw, gw, ow, bias, hgain)
        return pl.pallas_call(
            flush,
            out_shape=(
                jax.ShapeDtypeStruct(stream.shape, BF16),
                jax.ShapeDtypeStruct(states.shape, F32),
            ),
            in_specs=[pl.BlockSpec(memory_space=pltpu.VMEM)] * 2,
            out_specs=(hbm_spec,) * 2,
            scratch_shapes=[dma((1 + layers,))],
            compiler_params=pltpu.CompilerParams(vmem_limit_bytes=1024 * 1024),
            name="flush",
        )(new_stream, new_states)

    in_specs = (
        P("grp", "dp"),
        P(None, ("grp", "dp"), "tp", None, None),
        P(None, "dp"),
        P(None, "dp", "tp"),
        P(None, "dp", "tp"),
        P(None, "dp", "tp"),
        P(None, "dp", "tp"),
        P(None, "dp", "tp"),
        P(None, "dp", "tp"),
        P(None, "tp", "dp"),
        P(None, "tp"),
        P(None, "tp"),
    )
    out_specs = (P("grp", "dp"), P(None, ("grp", "dp"), "tp", None, None))
    return jax.shard_map(
        per_device, mesh=mesh, in_specs=in_specs, out_specs=out_specs, check_vma=False
    )
```
